32 devices in a mesh: sp: 4 (over z), fs: 4 (over y, x), tp: 2 (over core).
Axes of the slice: x: 2, y: 2, z: 4, core: 2. Of those that a mesh axis runs over, the one named last changes fastest.
Arguments:
- tokens: bfloat16 [8192, 2048], P(('fs', 'sp')), parts along dimension 0, may hold values from -6 to 6
- norm_gain: bfloat16 [2048], replicated, may hold values from 0.099609375 to 1.8984375
- w_query: bfloat16 [2048, 1024], P('sp', 'tp'), may hold values from -0.15625 to 0.15625
- w_key: bfloat16 [2048, 256], P('sp', 'tp'), may hold values from -0.15625 to 0.15625
- w_value: bfloat16 [2048, 256], P('sp', 'tp'), may hold values from -0.125 to 0.125
- w_glu_value: bfloat16 [2048, 1024], P('sp', 'tp'), may hold values from -0.22097087 to 0.22097087
- w_glu_gate: bfloat16 [2048, 1024], P('sp', 'tp'), may hold values from -0.125 to 0.125
- conv_taps: bfloat16 [31, 1024], P(None, 'tp'), may hold values from -1 to 1
- convolution_norm_gain: bfloat16 [1024], replicated, may hold values from 0.099609375 to 1.8984375
- head_gain: bfloat16 [128], replicated, may hold values from 0.099609375 to 1.8984375
- lam: float32 [8], P('tp'), may hold values from 0.3 to 0.8
- w_out: bfloat16 [2048, 2048], P(None, 'sp'), may hold values from -0.125 to 0.125
Outputs:
- mixed: bfloat16 [8192, 2048], P(('fs', 'sp', 'tp')), parts along dimension 0
- log_totals: float32 [8192, 16], P(('fs', 'sp'), 'tp'), parts along dimension 0
The draws below stay inside these ranges and needn't reach their ends.
There are 4 independent parts, one for each index of `fs`. The reference program is written for one: setup_inputs(seed, part) draws one part's arguments, and reference() takes and returns one part's arrays. A program takes and returns all parts, laid end to end along the dimension named above; an argument that names none is the same for every part. Nothing has to cross between parts.
All inputs are finite; a program needn't handle non-finite values.
Results may differ from the reference program's by a relative error of at most 0.0095.
Values may be sent and summed in bfloat16 or wider, within the bound.
A program may use at most 64 MiB of HBM per device.

```python
import math
import jax
import jax.numpy as jnp
from jax import lax

D = 2048
HEADS = 8
KV_HEADS = 2
QK = 64
VDIM = 128
CONV = 1024
KW = 31
SEQ = 2048


def draw_w_glu_value(key, part):
    first, second = jax.random.split(jax.random.fold_in(key, 41))
    placed = (jnp.arange(CONV, dtype=jnp.float32) + jax.random.uniform(first, (CONV,), jnp.float32)) / CONV
    column_scale = 10.0 ** placed / 4.0
    base = jax.random.truncated_normal(second, -4.0, 4.0, (D, CONV), jnp.float32)
    values = base * column_scale[None, :] * D ** (-0.5)
    return jnp.clip(values, -10.0 * D ** (-0.5), 10.0 * D ** (-0.5)).astype(jnp.bfloat16)


def block_scale(own_key, dims, cuts, low, high):
    def one(axis_at, shards_of):
        draws = jax.random.uniform(jax.random.fold_in(jax.random.fold_in(own_key, 6), axis_at), (shards_of,), jnp.float32, low / len(cuts), high / len(cuts))
        return jnp.repeat(jnp.exp(draws), dims[axis_at] // shards_of).reshape((-1,) + (1,) * (len(dims) - axis_at - 1))

    level = one(*cuts[0])
    for cut in cuts[1:]:
        level = level * one(*cut)
    return level


def bell_draw(key, extent, scale, limit, cuts=(), kind=jnp.bfloat16):
    entries = jax.random.normal(key, extent, jnp.float32) * scale
    if len(cuts) > 0:
        entries = block_scale(key, extent, cuts, -0.22, 0.18) * entries
    return jnp.clip(entries, min=-limit, max=limit).astype(kind)


def setup_inputs(seed: int = 0, part: int = 0) -> dict:
    streams_of = jax.random.split(jax.random.key(seed), 13)
    part_keys = jax.random.split(jax.random.fold_in(streams_of[12], part), 13)
    return {
        "tokens": bell_draw(part_keys[0], (SEQ, D), 1.0, 6.0, ((0, 4),)),
        "norm_gain": jnp.clip(1.0 + 0.18 * jax.random.normal(streams_of[1], (D,), jnp.float32), 0.099609375, 1.8984375).astype(jnp.bfloat16),
        "w_query": bell_draw(streams_of[2], (D, HEADS * 2 * QK), (D * 2 // 3) ** -0.5, 0.15625, ((0, 4), (1, 2))),
        "w_key": bell_draw(streams_of[3], (D, KV_HEADS * 2 * QK), (D * 2 // 3) ** -0.5, 0.15625, ((0, 4), (1, 2))),
        "w_value": bell_draw(streams_of[4], (D, KV_HEADS * VDIM), D ** -0.5, 0.125, ((0, 4), (1, 2))),
        "w_glu_value": draw_w_glu_value(jax.random.fold_in(streams_of[12], 71), part),
        "w_glu_gate": bell_draw(streams_of[6], (D, CONV), D ** -0.5, 0.125, ((0, 4), (1, 2))),
        "conv_taps": bell_draw(streams_of[7], (KW, CONV), KW ** -0.5, 1.0, ((1, 2),)),
        "convolution_norm_gain": jnp.clip(1.0 + 0.18 * jax.random.normal(streams_of[8], (CONV,), jnp.float32), 0.099609375, 1.8984375).astype(jnp.bfloat16),
        "head_gain": jnp.clip(1.0 + 0.18 * jax.random.normal(streams_of[9], (VDIM,), jnp.float32), 0.099609375, 1.8984375).astype(jnp.bfloat16),
        "lam": jnp.clip(0.3 + 0.5 * jax.random.uniform(streams_of[10], (HEADS,), jnp.float32) ** block_scale(streams_of[10], (HEADS,), ((0, 2),), -0.2, 0.2), 0.3, 0.8),
        "w_out": bell_draw(streams_of[11], (HEADS * VDIM + CONV, D), (HEADS * VDIM + CONV) ** -0.5, 0.125, ((1, 4),)),
    }


def reference(tokens, norm_gain, w_query, w_key, w_value, w_glu_value, w_glu_gate, conv_taps, convolution_norm_gain, head_gain, lam, w_out):
    length = tokens.shape[0]
    eps = 1e-06
    tok32 = tokens.astype(jnp.float32)
    normalized_rows = (tok32 * lax.rsqrt(lax.optimization_barrier(jnp.mean(tok32 * tok32, axis=-1, keepdims=True)) + eps) * norm_gain.astype(jnp.float32)).astype(jnp.bfloat16)
    queries = jnp.dot(normalized_rows, w_query, preferred_element_type=jnp.float32).astype(jnp.bfloat16)
    keys = jnp.dot(normalized_rows, w_key, preferred_element_type=jnp.float32).astype(jnp.bfloat16)
    values = jnp.dot(normalized_rows, w_value, preferred_element_type=jnp.float32).astype(jnp.bfloat16)
    glu_val = jnp.dot(normalized_rows, w_glu_value, preferred_element_type=jnp.float32)
    glu_gate = jnp.dot(normalized_rows, w_glu_gate, preferred_element_type=jnp.float32)
    gated = (glu_val * jax.nn.sigmoid(glu_gate)).astype(jnp.bfloat16)
    padded = jnp.concatenate([jnp.zeros((KW - 1, CONV), jnp.bfloat16), gated], axis=0)
    conv = jnp.zeros((length, CONV), jnp.float32)
    for tap in range(KW):
        conv = conv + conv_taps[tap].astype(jnp.float32) * padded[tap:tap + length].astype(jnp.float32)
    conv = conv.astype(jnp.bfloat16).astype(jnp.float32)
    conv_act = jax.nn.silu(conv * lax.rsqrt(lax.optimization_barrier(jnp.mean(conv * conv, axis=-1, keepdims=True)) + eps) * convolution_norm_gain.astype(jnp.float32)).astype(jnp.bfloat16)
    group = HEADS // KV_HEADS
    key_all = keys.astype(jnp.float32).reshape(length, KV_HEADS, 2, QK)
    value_rows_full = values.astype(jnp.float32).reshape(length, KV_HEADS, VDIM)
    block = math.gcd(length, 512)
    query_blocks = queries.reshape(length // block, block, KV_HEADS, group, 2, QK)
    key_pos = jnp.arange(length, dtype=jnp.int32)

    def one_block(item):
        query_block, index = item
        qfloat = query_block.astype(jnp.float32)
        score = jnp.einsum('tkgmd,nkmd->tkgmn', qfloat, key_all) * QK ** (-0.5)
        query_pos = index * block + jnp.arange(block, dtype=jnp.int32)
        allowed = key_pos[None, None, None, None, :] <= query_pos[:, None, None, None, None]
        weight = jnp.where(allowed, jnp.exp(score), 0.0)
        total = lax.optimization_barrier(jnp.sum(weight, axis=-1))
        rounded_values = weight.astype(jnp.bfloat16).astype(jnp.float32)
        running_total = jnp.einsum('doejz,zow->doejw', rounded_values, value_rows_full)
        return (running_total, total)
    running_total, total = lax.map(one_block, (query_blocks, jnp.arange(length // block, dtype=jnp.int32)))
    running_total = running_total.reshape(length, HEADS, 2, VDIM)
    total = total.reshape(length, HEADS, 2)
    lam32 = lam.astype(jnp.float32)
    diff = running_total[:, :, 0] / total[:, :, 0, None] - lam32[None, :, None] * running_total[:, :, 1] / total[:, :, 1, None]
    att_out = diff * lax.rsqrt(lax.optimization_barrier(jnp.mean(diff * diff, axis=-1, keepdims=True)) + eps) * head_gain.astype(jnp.float32)
    att_out = att_out.astype(jnp.bfloat16).reshape(length, HEADS * VDIM)
    log_totals = jnp.log(total).reshape(length, HEADS * 2)
    both = jnp.concatenate([att_out, conv_act], axis=1)
    mixed = jnp.dot(both, w_out, preferred_element_type=jnp.float32).astype(jnp.bfloat16)
    return (mixed, log_totals)
```

```python
import functools
import math

import jax
import jax.numpy as jnp
from jax import lax
from jax.experimental import pallas as pl
from jax.experimental.pallas import tpu as pltpu
from jax.sharding import PartitionSpec as P

QK = 64
VDIM = 128
EPS = 1e-06
MESH = pl.DeviceIdType.MESH
BF = jnp.bfloat16
F32 = jnp.float32
LANES = 128
RIM = 32
WIDE = 256
TOKEN_CUTS = 4


def kernel(
    n,
    conv_total,
    tok_h,
    gain_r,
    wq_h,
    wk_h,
    wv_h,
    wgv_h,
    wgg_h,
    taps_r,
    cgain_r,
    hgain_r,
    lam_r,
    wo_h,
    mixed_r,
    log_r,
    tok,
    normed,
    gkv,
    gq,
    gb,
    gc,
    q2,
    kvb,
    acc,
    gated,
    rim,
    pad,
    conv,
    taps_in,
    taps_f,
    lam_in,
    lam_s,
    sq_own,
    sq_in,
    both,
    part_out,
    part_in,
    keep,
    lsrc,
    ldst,
    loc,
    zs,
    pr,
    ys,
    ds,
    dr,
    kzs,
    kzr,
    kds,
    kdr,
    tks,
    tkr,
    rims,
    rimr,
    sqs,
    smalls,
    ps,
    prs,
    ls,
    lr,
):
    s = lax.axis_index("sp")
    f = lax.axis_index("fs")
    t = lax.axis_index("tp")
    fx = f + 1 - 2 * (f % 2)
    fy = (f + 2) % 4
    hx = f % 2
    hy = (f // 2) % 2
    native = t == hx
    guest = t != hx
    ph = jnp.where(native, hy, 1 - hy)

    def dev(sp, fs, tp):
        return {"sp": sp, "fs": fs, "tp": tp}

    left = dev(s - 1, f, t)
    right = dev(s + 1, f, t)
    xdev = dev(s, fx, t)
    mate = dev(s, f, 1 - t)
    ydev = dev(s, fy, 1 - t)
    heads = lam_r.shape[1]
    rows, width = tok.shape
    hr = rows // 2
    nb, chans = gb.shape[0], gated.shape[2] * gb.shape[0]
    nc = gc.shape[0]
    oc = gc.shape[3]
    att_rows = heads * VDIM
    has_left = s > 0
    has_right = s < n - 1
    groups = [(gkv, None), (gq, None)]
    groups += [(gb, i) for i in range(nb)] + [(gc, i) for i in range(nc)]
    first_c = 2 + nb

    def slab(g, o):
        buf, i = groups[g]
        return buf.at[o] if i is None else buf.at[i, o]

    def chunk(g, o, half):
        buf, i = groups[g]
        size = buf.shape[-2] // 2
        at = pl.ds(pl.multiple_of(half * size, size), size)
        return buf.at[o, at, :] if i is None else buf.at[i, o, at, :]

    def remote(src, dst, ss, rs, to):
        return pltpu.make_async_remote_copy(src, dst, ss, rs, device_id=to, device_id_type=MESH)

    loads = {}
    count = [0]

    def load(g, a, b):
        c = pltpu.make_async_copy(a, b, loc.at[count[0]])
        count[0] += 1
        loads.setdefault(g, []).append(c)

    load(0, wk_h, gkv.at[s, :, pl.ds(0, LANES)])
    load(0, wv_h, gkv.at[s, :, pl.ds(LANES, LANES)])
    load(1, wq_h, gq.at[s])
    for i in range(nb):
        load(2 + i, wgv_h.at[:, pl.ds(i * WIDE, WIDE)], gb.at[i, s, :, pl.ds(0, WIDE)])
        load(2 + i, wgg_h.at[:, pl.ds(i * WIDE, WIDE)], gb.at[i, s, :, pl.ds(WIDE, WIDE)])
    for i in range(nc):
        cols = pl.ds(i * oc, oc)
        a_rows = pl.ds(pl.multiple_of(hx * att_rows, att_rows), att_rows)
        c_rows = pl.ds(pl.multiple_of(2 * att_rows + hx * chans, chans), chans)
        load(first_c + i, wo_h.at[a_rows, cols], gc.at[i, s, pl.ds(0, att_rows), :])
        load(first_c + i, wo_h.at[c_rows, cols], gc.at[i, s, pl.ds(att_rows, chans), :])
    my_rows = pl.multiple_of(t * hr, hr)
    tok_load = pltpu.make_async_copy(tok_h.at[pl.ds(my_rows, hr), :], tok.at[pl.ds(0, hr), :], loc.at[count[0]])

    @pl.when(native)
    def _():
        for g in range(2):
            for c in loads[g]:
                c.start()

    tok_load.start()

    @pl.when(native)
    def _():
        for g in range(2, first_c):
            for c in loads[g]:
                c.start()

    for g in range(first_c, len(groups)):
        for c in loads[g]:
            c.start()

    bar = pltpu.get_barrier_semaphore()
    for to in (mate, ydev, dev(s, fx, 0), dev(s, fx, 1)):
        pl.semaphore_signal(bar, 1, device_id=to, device_id_type=MESH)

    @pl.when(has_left)
    def _():
        for e in range(2):
            pl.semaphore_signal(bar, 1, device_id=dev(s - 1, f, e), device_id_type=MESH)

    @pl.when(has_right)
    def _():
        for e in range(2):
            pl.semaphore_signal(bar, 1, device_id=dev(s + 1, f, e), device_id_type=MESH)

    pl.semaphore_wait(bar, 4 + jnp.where(has_left, 2, 0) + jnp.where(has_right, 2, 0))

    cut = hr // TOKEN_CUTS
    swaps = [
        remote(
            tok_h.at[pl.ds(pl.multiple_of(my_rows + i * cut, cut), cut), :],
            tok.at[pl.ds(hr + i * cut, cut), :],
            tks.at[i],
            tkr.at[i],
            xdev,
        )
        for i in range(TOKEN_CUTS)
    ]
    for c in swaps:
        c.start()

    def zcopy(g, o, right_way):
        c = chunk(g, o, hy)
        return remote(c, c, zs.at[g, 0 if right_way else 1, o], pr.at[g, o], right if right_way else left)

    def pcopy(g, o):
        c = chunk(g, o, ph)
        return remote(c, c, ys.at[g, o], pr.at[g, o], ydev)

    def dcopy(g, o, half):
        c = chunk(g, o, half)
        return remote(c, c, ds.at[g, o], dr.at[g, o], mate)

    def own_dcopy(g):
        c = slab(g, s)
        return remote(c, c, ds.at[g, s], dr.at[g, s], mate)

    def sides(k, fn):
        @pl.when(s >= k)
        def _():
            fn(s - k, True)

        @pl.when(s + k < n)
        def _():
            fn(s + k, False)

    def own_send(g):
        @pl.when(native)
        def _():
            for c in loads[g]:
                c.wait()

            @pl.when(has_right)
            def _():
                zcopy(g, s, True).start()

            @pl.when(has_left)
            def _():
                zcopy(g, s, False).start()

            if g < first_c:
                own_dcopy(g).start()

        if g >= first_c:

            @pl.when(guest)
            def _():
                for c in loads[g]:
                    c.wait()

    def primary(g, k):
        def go(o, right_way):
            pcopy(g, o).wait_recv()

            @pl.when(native)
            def _():
                @pl.when(has_right if right_way else has_left)
                def _():
                    zcopy(g, o, right_way).start()

                pcopy(g, o).start()

            dcopy(g, o, ph).start()

        sides(k, go)

    def arrived_one(g, k):
        sides(k, lambda o, _: dcopy(g, o, 1 - ph).wait_recv())

    def arrived_own(g):
        if g < first_c:

            @pl.when(guest)
            def _():
                own_dcopy(g).wait_recv()

    def arrived(g):
        arrived_own(g)
        for k in range(1, n):
            arrived_one(g, k)

    def drain(g):
        @pl.when(native)
        def _():
            @pl.when(has_right)
            def _():
                zcopy(g, s, True).wait_send()

            @pl.when(has_left)
            def _():
                zcopy(g, s, False).wait_send()

            if g < first_c:
                own_dcopy(g).wait_send()

        for k in range(1, n):

            def go(o, right_way):
                @pl.when(native)
                def _():
                    pcopy(g, o).wait_send()

                    @pl.when(has_right if right_way else has_left)
                    def _():
                        zcopy(g, o, right_way).wait_send()

                dcopy(g, o, ph).wait_send()

            sides(k, go)

    def kv_at(j, o, half):
        return kvb.at[j, o, pl.ds(pl.multiple_of(half * hr, hr), hr), :]

    def kv_right(j, o):
        c = kv_at(j, o, t)
        return remote(c, c, kzs.at[j, o], kzr.at[j, o], right)

    def kv_mate(j, o, half):
        c = kv_at(j, o, half)
        return remote(c, c, kds.at[j, o], kdr.at[j, o], mate)

    def kv_send(j, o):
        @pl.when(has_right)
        def _():
            kv_right(j, o).start()

        kv_mate(j, o, t).start()

    def kv_take(j, k):
        @pl.when(s >= k)
        def _():
            kv_right(j, s - k).wait_recv()
            kv_send(j, s - k)

    items = [(g, k) for g in range(len(groups)) for k in range(1, n)]
    per = n - 1
    state = {"at": 0}

    def advance(g, part=1.0):
        to = min(len(items), g * per + math.ceil(part * per - 1e-6))
        for i in range(state["at"], to):
            primary(*items[i])
            if (i + 1) % per == 0 and items[i][0] + 2 < len(groups):
                own_send(items[i][0] + 2)
        state["at"] = max(state["at"], to)

    tall = min(256, hr)
    per_map = hr // tall
    per_head = 2 * per_map

    def attend_part(j, o, diagonal, lo, hi):
        kx = kvb[j, o, :, :LANES]
        vx = jnp.concatenate([kvb[j, o, :, LANES:], jnp.ones((rows, VDIM), BF)], axis=1)

        def step(i, carry):
            h = i // per_head
            at = pl.multiple_of((i % per_head) * tall, tall)
            score = lax.dot_general(
                q2[j, h, pl.ds(at, tall), :],
                kx,
                (((1,), (1,)), ((), ())),
                preferred_element_type=F32,
            )
            w = jnp.exp2(score * (QK**-0.5 * math.log2(math.e)))
            if diagonal:
                pos = t * hr + (at % hr) + lax.broadcasted_iota(jnp.int32, w.shape, 0)
                w = jnp.where(lax.broadcasted_iota(jnp.int32, w.shape, 1) <= pos, w, 0.0)
            pv = jnp.dot(w.astype(BF), vx, preferred_element_type=F32)
            if diagonal:
                acc[j, h, pl.ds(at, tall), :] = pv
            else:
                acc[j, h, pl.ds(at, tall), :] += pv
            return carry

        lax.fori_loop(lo * per_head, hi * per_head, step, 0, unroll=2)

    def attend_self(j, between):
        kv_mate(j, s, 1 - t).wait_recv()
        attend_part(j, s, True, 0, heads // 2)
        between()
        attend_part(j, s, True, heads // 2, heads)

    def attend_back(j, k, between):
        @pl.when(s >= k)
        def _():
            kv_mate(j, s - k, 1 - t).wait_recv()
            attend_part(j, s - k, False, 0, heads // 2)

        between()

        @pl.when(s >= k)
        def _():
            attend_part(j, s - k, False, heads // 2, heads)

    own_send(0)
    own_send(1)
    taps_copy = remote(taps_r, taps_in, smalls.at[0], smalls.at[1], mate)
    lam_copy = remote(lam_r, lam_in, smalls.at[2], smalls.at[3], mate)

    @pl.when(native)
    def _():
        taps_copy.start()
        lam_copy.start()
        taps_f[...] = taps_r[...].astype(F32)
        lam_s[...] = lam_r[...]

    gain = gain_r[...].reshape(1, width).astype(F32)

    def norm_step(i, carry):
        at = pl.ds(pl.multiple_of(i * 32, 32), 32)
        x = tok[at, :].astype(F32)
        r = lax.rsqrt(jnp.mean(x * x, axis=-1, keepdims=True) + EPS)
        normed[at, :] = (x * r * gain).astype(BF)
        return carry

    def norm_rows(lo, hi):
        lax.fori_loop(lo // 32, hi // 32, norm_step, 0)

    def project_kv(j):
        kv = jnp.dot(
            normed[j * hr : (j + 1) * hr, :],
            gkv[...].reshape(width, 2 * LANES),
            preferred_element_type=F32,
        ).astype(BF)
        kvb[j, s, pl.ds(my_rows, hr), :] = kv
        kv_send(j, s)

    lane = lax.broadcasted_iota(jnp.int32, (hr, LANES), 1)

    def project_q(j):
        def q_step(h, carry):
            cols = pl.ds(pl.multiple_of(h * 2 * LANES, 2 * LANES), 2 * LANES)
            q = jnp.dot(
                normed[j * hr : (j + 1) * hr, :],
                gq[:, :, cols].reshape(width, 2 * LANES),
                preferred_element_type=F32,
            )
            for e in range(2):
                one = q[:, e * LANES : (e + 1) * LANES]
                q2[j, 2 * h + e, :hr, :] = jnp.where(lane < QK, one, 0.0).astype(BF)
                q2[j, 2 * h + e, hr:, :] = jnp.where(lane >= QK, one, 0.0).astype(BF)
            return carry

        lax.fori_loop(0, heads // 2, q_step, 0)

    def rim_copy(i, to, e):
        return remote(
            gated.at[i, pl.ds(hr - RIM, RIM), :] if e == 0 else gated.at[i, pl.ds(rows - RIM, RIM), :],
            rim.at[i, e],
            rims.at[i, e],
            rimr.at[i, e],
            to,
        )

    def glu(i):
        for j in range(2):
            at = slice(j * hr, (j + 1) * hr)
            val = jnp.dot(normed[at, :], gb[i, :, :, :WIDE].reshape(width, WIDE), preferred_element_type=F32)
            gate = jnp.dot(normed[at, :], gb[i, :, :, WIDE:].reshape(width, WIDE), preferred_element_type=F32)
            g = (val * jax.nn.sigmoid(gate)).astype(BF)
            gated[i, at, :] = g
            pad[j, RIM:, i * WIDE : (i + 1) * WIDE] = g.astype(F32)
        for e in range(2):

            @pl.when(t == 0)
            def _():
                rim_copy(i, mate, e).start()

            @pl.when((t == 1) & has_right)
            def _():
                rim_copy(i, dev(s + 1, f, 0), e).start()

    taps = taps_r.shape[0]
    shift = RIM - (taps - 1)
    tile = min(128, hr)
    wants_rim = (t == 1) | has_left

    def convolve(i):
        @pl.when(wants_rim)
        def _():
            for e in range(2):
                rim_copy(i, mate, e).wait_recv()
                pad[e, :RIM, i * WIDE : (i + 1) * WIDE] = rim[i, e].astype(F32)

        @pl.when((t == 0) & (s == 0))
        def _():
            pad[:, :RIM, i * WIDE : (i + 1) * WIDE] = jnp.zeros((2, RIM, WIDE), F32)

        def conv_step(m, carry):
            cols = pl.ds(pl.multiple_of(i * WIDE + (m // 2) * LANES, LANES), LANES)
            j = m % 2
            for r in range(0, hr, tile):
                total = jnp.zeros((tile, LANES), F32)
                for p in range(taps):
                    total = total + taps_f[p : p + 1, cols] * pad[j, r + shift + p : r + shift + p + tile, cols]
                conv[pl.ds(pl.multiple_of(j * hr + r, tile), tile), cols] = total.astype(BF).astype(F32)
            return carry

        lax.fori_loop(0, 2 * WIDE // LANES, conv_step, 0)

    sq_copy = remote(sq_own, sq_in, sqs.at[0], sqs.at[1], xdev)

    def square_sums():
        cv = conv[...]
        sums = jnp.broadcast_to(jnp.sum(cv * cv, axis=-1, keepdims=True), (rows, LANES))
        sq_own[...] = sums.T[:8, :]
        sq_copy.start()

    def conv_out():
        sq_copy.wait()
        other = jnp.concatenate([sq_in[:, hr:], sq_in[:, :hr]], axis=1)
        inv = lax.rsqrt((sq_own[...] + other) / conv_total + EPS)
        inv = jnp.broadcast_to(inv[:1, :], (LANES, rows)).T[:, :1]
        cgain = cgain_r[pl.ds(pl.multiple_of(hx * chans, LANES), chans)].reshape(1, chans).astype(F32)
        both[:, att_rows:] = jax.nn.silu(conv[...] * inv * cgain).astype(BF)

    def head_rows(j):
        def go(i, carry):
            at = pl.multiple_of(i * tile, tile)
            ids = lax.broadcasted_iota(jnp.int32, (tile, LANES), 1)
            logs = jnp.zeros((tile, LANES), F32)
            for h in range(heads):
                a0 = acc[j, h, pl.ds(at, tile), :]
                a1 = acc[j, h, pl.ds(pl.multiple_of(hr + at, tile), tile), :]
                t0, t1 = a0[:, VDIM:], a1[:, VDIM:]
                diff = a0[:, :VDIM] / t0 - lam_s[:, h : h + 1] * (a1[:, :VDIM] / t1)
                out = (
                    diff
                    * lax.rsqrt(jnp.mean(diff * diff, axis=-1, keepdims=True) + EPS)
                    * hgain_r[...].astype(F32)
                )
                both[pl.ds(pl.multiple_of(j * hr + at, tile), tile), h * VDIM : (h + 1) * VDIM] = out.astype(BF)
                logs = jnp.where(ids == 2 * h, jnp.log(t0), logs)
                logs = jnp.where(ids == 2 * h + 1, jnp.log(t1), logs)
            lsrc[j, :, pl.ds(at, tile)] = logs.T[: 2 * heads, :]
            return carry

        lax.fori_loop(0, hr // tile, go, 0)

    log_mate = remote(lsrc.at[0], ldst.at[t], ls.at[0], lr.at[t], mate)
    log_x = remote(lsrc.at[1], ldst.at[t], ls.at[1], lr.at[t], dev(s, fx, hx))

    def send_logs():
        log_x.start()

        @pl.when(guest)
        def _():
            log_mate.start()

    def take_logs():
        @pl.when(native)
        def _():
            log_r[:, pl.ds(my_rows, hr)] = lsrc[0]
            remote(lsrc.at[0], ldst.at[1 - t], ls.at[0], lr.at[1 - t], mate).wait_recv()
            log_r[:, pl.ds(pl.multiple_of((1 - t) * hr, hr), hr)] = ldst[1 - t]

        @pl.when(guest)
        def _():
            for e in range(2):
                remote(lsrc.at[1], ldst.at[e], ls.at[1], lr.at[e], mate).wait_recv()
                log_r[:, e * hr : (e + 1) * hr] = ldst[e]
            log_mate.wait_send()

        log_x.wait_send()

    def xcopy(i, o):
        return remote(part_out.at[i, o], part_in.at[i, o], ps.at[i, o], prs.at[i, o], xdev)

    def out_block(i, o):
        part_out[i, o] = jnp.dot(both[hr:, :], gc[i, o], preferred_element_type=F32).astype(BF)
        xcopy(i, o).start()
        keep[i, o] = jnp.dot(both[:hr, :], gc[i, o], preferred_element_type=F32)

    def finish(i):
        def go(o, carry):
            xcopy(i, o).wait_recv()
            xcopy(i, o).wait_send()
            mixed_r[:, pl.ds(pl.multiple_of((o * nc + i) * oc, oc), oc)] = (
                keep[i, o] + part_in[i, o].astype(F32)
            ).astype(BF)
            return carry

        lax.fori_loop(0, n, go, 0)

    def nothing():
        pass

    tok_load.wait()
    norm_rows(0, hr)
    advance(0)
    arrived(0)
    project_kv(0)
    advance(1)
    arrived(1)
    project_q(0)
    attend_self(0, lambda: advance(2, 0.4))
    kv_take(0, 1)
    for i in range(TOKEN_CUTS):
        swaps[i].wait_recv()
        norm_rows(hr + i * cut, hr + (i + 1) * cut)
    project_kv(1)
    project_q(1)
    advance(2, 0.7)
    attend_self(1, nothing)
    advance(2)
    if n > 2:
        kv_take(0, 2)
    kv_take(1, 1)
    attend_back(0, 1, lambda: advance(3, 0.4))
    attend_back(1, 1, lambda: advance(3, 0.7))
    arrived(2)

    @pl.when(guest)
    def _():
        taps_copy.wait_recv()
        lam_copy.wait_recv()
        taps_f[...] = taps_in[...].astype(F32)
        lam_s[...] = lam_in[...]

    glu(0)
    advance(3)
    if n > 2:
        kv_take(1, 2)
        attend_back(0, 2, lambda: advance(4, 0.4))
    for i in range(1, nb):
        arrived(2 + i)
        glu(i)
    if n > 2:
        attend_back(1, 2, lambda: advance(4, 0.7))
    for k in range(3, n):
        kv_take(0, k)
        kv_take(1, k)
    for i in range(nb):
        convolve(i)
    square_sums()
    advance(4)
    for k in range(3, n):
        attend_back(1, k, nothing)
    head_rows(1)
    advance(5, 0.4)
    for k in range(3, n):
        attend_back(0, k, nothing)
    head_rows(0)
    send_logs()
    conv_out()
    own_wait = nothing
    for i in range(nc):
        out_block(i, s)
    for i in range(nc):
        for k in range(1, n):
            advance(first_c + i, k / per)
            arrived_one(first_c + i, k)
            sides(k, lambda o, _: out_block(i, o))
    take_logs()
    for i in range(nc):
        finish(i)

    for g in range(len(groups)):
        drain(g)
    for c in swaps:
        c.wait_send()
    for e in range(2):
        for i in range(nb):

            @pl.when((t == 0) | has_right)
            def _():
                rim_copy(i, mate, e).wait_send()

    @pl.when(native)
    def _():
        taps_copy.wait_send()
        lam_copy.wait_send()

    for j in range(2):
        for k in range(n):

            @pl.when(s >= k)
            def _():
                kv_mate(j, s - k, t).wait_send()

                @pl.when(has_right)
                def _():
                    kv_right(j, s - k).wait_send()


def body(n, conv_total, tokens, norm_gain, w_query, w_key, w_value, w_gv, w_gg, taps, cgain, hgain, lam, w_out):
    rows, width = tokens.shape
    heads = lam.shape[0]
    chans = w_gv.shape[1]
    qcols = w_query.shape[1]
    wrows = w_query.shape[0]
    ocols = w_out.shape[1]
    half = rows // 2
    nb = chans // WIDE
    nc = max(1, ocols // WIDE)
    oc = ocols // nc
    feats = heads * VDIM + chans
    ng = 2 + nb + nc
    any_ = pl.BlockSpec(memory_space=pl.ANY)
    vm = pl.BlockSpec(memory_space=pltpu.VMEM)
    dma = pltpu.SemaphoreType.DMA
    v = pltpu.VMEM
    mixed, logs = pl.pallas_call(
        functools.partial(kernel, n, conv_total),
        out_shape=(
            jax.ShapeDtypeStruct((half, width), BF),
            jax.ShapeDtypeStruct((2 * heads, rows), F32),
        ),
        in_specs=[any_, vm, any_, any_, any_, any_, any_, vm, vm, vm, vm, any_],
        out_specs=(vm, vm),
        scratch_shapes=[
            v((rows, width), BF),
            v((rows, width), BF),
            v((n, wrows, 2 * LANES), BF),
            v((n, wrows, qcols), BF),
            v((nb, n, wrows, 2 * WIDE), BF),
            v((nc, n, feats, oc), BF),
            v((2, heads, 2 * half, LANES), BF),
            v((2, n, rows, 2 * LANES), BF),
            v((2, heads, 2 * half, 2 * VDIM), F32),
            v((nb, rows, WIDE), BF),
            v((nb, 2, RIM, WIDE), BF),
            v((2, RIM + half, chans), F32),
            v((rows, chans), F32),
            v(taps.shape, BF),
            v(taps.shape, F32),
            v((1, heads), F32),
            v((1, heads), F32),
            v((8, rows), F32),
            v((8, rows), F32),
            v((rows, feats), BF),
            v((nc, n, half, oc), BF),
            v((nc, n, half, oc), BF),
            v((nc, n, half, oc), F32),
            v((2, 2 * heads, half), F32),
            v((2, 2 * heads, half), F32),
            dma((4 + 2 * nb + 2 * nc,)),
            dma((ng, 2, n)),
            dma((ng, n)),
            dma((ng, n)),
            dma((ng, n)),
            dma((ng, n)),
            dma((2, n)),
            dma((2, n)),
            dma((2, n)),
            dma((2, n)),
            dma((TOKEN_CUTS,)),
            dma((TOKEN_CUTS,)),
            dma((nb, 2)),
            dma((nb, 2)),
            dma((2,)),
            dma((4,)),
            dma((nc, n)),
            dma((nc, n)),
            dma((2,)),
            dma((2,)),
        ],
        compiler_params=pltpu.CompilerParams(
            collective_id=0, has_side_effects=True, vmem_limit_bytes=60 * 1024 * 1024
        ),
    )(
        tokens,
        norm_gain,
        w_query,
        w_key,
        w_value,
        w_gv,
        w_gg,
        taps,
        cgain,
        hgain.reshape(1, -1),
        lam.reshape(1, -1),
        w_out,
    )
    return mixed, logs.T


def solution(mesh):
    n = mesh.shape["sp"]

    def run(*args):
        return body(n, args[8].shape[0], *args)

    return jax.shard_map(
        run,
        mesh=mesh,
        in_specs=(
            P(("fs", "sp"), None),
            P(),
            P("sp", "tp"),
            P("sp", "tp"),
            P("sp", "tp"),
            P("sp", "tp"),
            P("sp", "tp"),
            P(None, "tp"),
            P(),
            P(),
            P("tp"),
            P(None, "sp"),
        ),
        out_specs=(P(("fs", "sp", "tp"), None), P(("fs", "sp"), "tp")),
        check_vma=False,
    )
```

```python
import functools
import math

import jax
import jax.numpy as jnp
from jax import lax
from jax.experimental import pallas as pl
from jax.experimental.pallas import tpu as pltpu
from jax.sharding import PartitionSpec as P

QK = 64
VDIM = 128
EPS = 1e-06
MESH = pl.DeviceIdType.MESH
BF = jnp.bfloat16
F32 = jnp.float32
LANES = 128
RIM = 32
LOOK = 2
LAG = 2
AT = 0
WIDE = 256


def kernel(
    n,
    conv_total,
    tok_h,
    gain_r,
    wq_h,
    wk_h,
    wv_h,
    wgv_h,
    wgg_h,
    taps_r,
    cgain_r,
    hgain_r,
    lam_r,
    wo_h,
    mixed_r,
    log_r,
    tok,
    normed,
    gkv,
    gq,
    gb,
    gc,
    q2,
    kbuf,
    vbuf,
    acc,
    gated,
    rim,
    pad,
    conv,
    sq_own,
    sq_in,
    both,
    part_out,
    part_in,
    keep,
    loc,
    zs,
    zr,
    zu,
    zv,
    xs,
    xr,
    ys,
    yr,
    hxs,
    hxr,
    hys,
    hyr,
    kvs,
    kvr,
    rims,
    sqs,
    ps,
    pr,
):
    s = lax.axis_index("sp")
    f = lax.axis_index("fs")
    t = lax.axis_index("tp")
    fx = f + 1 - 2 * (f % 2)
    fy = (f + 2) % 4
    left = {"sp": s - 1, "fs": f, "tp": t}
    right = {"sp": s + 1, "fs": f, "tp": t}
    xdev = {"sp": s, "fs": fx, "tp": t}
    ydev = {"sp": s, "fs": fy, "tp": t}
    mate = {"sp": s, "fs": f, "tp": 1 - t}
    rows, width = tok.shape
    heads = lam_r.shape[0]
    chans = gated.shape[1]
    qcols = wq_h.shape[1]
    half = rows // 2
    nb, nc, oc = gb.shape[0], gc.shape[0], gc.shape[3]
    groups = [(gkv, None), (gq, None)]
    groups += [(gb, i) for i in range(nb)] + [(gc, i) for i in range(nc)]
    first_c = 2 + nb
    ng = first_c + nc
    twice = ng - 1
    has_left = s > 0
    has_right = s < n - 1

    d_rows = wq_h.shape[0]
    att_rows = heads * VDIM
    loads = {}
    count = [0]

    def load(g, src, dst):
        c = pltpu.make_async_copy(src, dst, loc.at[count[0]])
        count[0] += 1
        loads.setdefault(g, []).append(c)
        c.start()

    load(0, wk_h, gkv.at[s, :, pl.ds(0, LANES)])
    load(0, wv_h, gkv.at[s, :, pl.ds(LANES, LANES)])
    load(1, wq_h, gq.at[s])
    load("tok", tok_h, tok)
    for i in range(nb):
        load(2 + i, wgv_h.at[:, pl.ds(i * WIDE, WIDE)], gb.at[i, s, :, pl.ds(0, WIDE)])
        load(2 + i, wgg_h.at[:, pl.ds(i * WIDE, WIDE)], gb.at[i, s, :, pl.ds(WIDE, WIDE)])
    for i in range(nc):
        cols = pl.ds(i * oc, oc)
        a_rows = pl.ds(pl.multiple_of(t * att_rows, att_rows), att_rows)
        c_rows = pl.ds(pl.multiple_of(2 * att_rows + t * chans, chans), chans)
        load(first_c + i, wo_h.at[a_rows, cols], gc.at[i, s, pl.ds(0, att_rows), :])
        load(first_c + i, wo_h.at[c_rows, cols], gc.at[i, s, pl.ds(att_rows, chans), :])

    bar = pltpu.get_barrier_semaphore()
    for dev in (xdev, ydev, mate):
        pl.semaphore_signal(bar, 1, device_id=dev, device_id_type=MESH)

    @pl.when(has_left)
    def _():
        pl.semaphore_signal(bar, 1, device_id=left, device_id_type=MESH)

    @pl.when(has_right)
    def _():
        pl.semaphore_signal(bar, 1, device_id=right, device_id_type=MESH)

    pl.semaphore_wait(bar, 3 + jnp.where(has_left, 1, 0) + jnp.where(has_right, 1, 0))

    def chunk(g, o, q, part=None):
        buf, i = groups[g]
        size = buf.shape[-2] // 4
        if part is not None:
            size = size // 2
            q = q * 2 + part
        at = pl.ds(pl.multiple_of(q * size, size), size)
        return buf.at[o, at, :] if i is None else buf.at[i, o, at, :]

    def zcopy(g, o, right_way):
        c = chunk(g, o, f)
        return pltpu.make_async_remote_copy(
            c,
            c,
            zs.at[g, 0 if right_way else 1, o],
            zr.at[g, o],
            device_id=right if right_way else left,
            device_id_type=MESH,
        )

    def xcopy(g, o, q):
        c = chunk(g, o, q)
        return pltpu.make_async_remote_copy(
            c, c, xs.at[g, o], xr.at[g, o], device_id=xdev, device_id_type=MESH
        )

    def ycopy(g, o, q):
        c = chunk(g, o, q)
        return pltpu.make_async_remote_copy(
            c, c, ys.at[g, o], yr.at[g, o], device_id=ydev, device_id_type=MESH
        )

    def hxcopy(g, o, q):
        c = chunk(g, o, q, 0)
        return pltpu.make_async_remote_copy(
            c, c, hxs.at[g, o], hxr.at[g, o], device_id=xdev, device_id_type=MESH
        )

    def hycopy(g, o, q):
        c = chunk(g, o, q, 1)
        return pltpu.make_async_remote_copy(
            c, c, hys.at[g, o], hyr.at[g, o], device_id=ydev, device_id_type=MESH
        )

    fd = 3 - f

    def ucopy(o, right_way):
        c = chunk(twice, o, fd)
        return pltpu.make_async_remote_copy(
            c,
            c,
            zu.at[0 if right_way else 1, o],
            zv.at[o],
            device_id=right if right_way else left,
            device_id_type=MESH,
        )

    def sides(k, fn):
        @pl.when(s >= k)
        def _():
            fn(s - k, True)

        @pl.when(s + k < n)
        def _():
            fn(s + k, False)

    def own_send(g):
        for c in loads[g]:
            c.wait()

        @pl.when(has_right)
        def _():
            zcopy(g, s, True).start()
            if g == twice:
                ucopy(s, True).start()

        @pl.when(has_left)
        def _():
            zcopy(g, s, False).start()
            if g == twice:
                ucopy(s, False).start()

    def stage1(g, k):
        def go(o, right_way):
            zcopy(g, o, right_way).wait_recv()
            xcopy(g, o, f).start()
            ycopy(g, o, f).start()

            @pl.when(has_right if right_way else has_left)
            def _():
                zcopy(g, o, right_way).start()

            if g == twice:
                ucopy(o, right_way).wait_recv()

                @pl.when(has_right if right_way else has_left)
                def _():
                    ucopy(o, right_way).start()

        sides(k, go)

    def stage2(g, k):
        if g == twice:
            return

        def go(o, right_way):
            xcopy(g, o, fx).wait_recv()
            hycopy(g, o, fx).start()
            ycopy(g, o, fy).wait_recv()
            hxcopy(g, o, fy).start()

        sides(k, go)

    def stage3(g, k):
        def go(o, right_way):
            if g == twice:
                xcopy(g, o, fx).wait_recv()
                ycopy(g, o, fy).wait_recv()
                return
            hxcopy(g, o, fd).wait_recv()
            hycopy(g, o, fd).wait_recv()

        sides(k, go)

    def drain(g):
        @pl.when(has_right)
        def _():
            zcopy(g, s, True).wait_send()
            if g == twice:
                ucopy(s, True).wait_send()

        @pl.when(has_left)
        def _():
            zcopy(g, s, False).wait_send()
            if g == twice:
                ucopy(s, False).wait_send()

        for k in range(1, n):

            def go(o, right_way):
                xcopy(g, o, f).wait_send()
                ycopy(g, o, f).wait_send()
                if g != twice:
                    hycopy(g, o, fx).wait_send()
                    hxcopy(g, o, fy).wait_send()

                @pl.when(has_right if right_way else has_left)
                def _():
                    zcopy(g, o, right_way).wait_send()
                    if g == twice:
                        ucopy(o, right_way).wait_send()

            sides(k, go)

    def kvcopy(o):
        return [
            pltpu.make_async_remote_copy(
                b.at[o], b.at[o], kvs.at[i, o], kvr.at[i, o], device_id=right, device_id_type=MESH
            )
            for i, b in enumerate((kbuf, vbuf))
        ]

    def kv_take(k):
        @pl.when(s >= k)
        def _():
            for c in kvcopy(s - k):
                c.wait_recv()

            @pl.when(has_right)
            def _():
                for c in kvcopy(s - k):
                    c.start()

    tall = min(256, rows)
    per_head = 2 * rows // tall

    def attend(o, diagonal, lo, hi):
        vx = jnp.concatenate([vbuf[o], jnp.ones((rows, VDIM), BF)], axis=1)
        kx = kbuf[o]

        def step(i, carry):
            h = i // per_head
            at = pl.multiple_of((i % per_head) * tall, tall)
            score = lax.dot_general(
                q2[h, pl.ds(at, tall), :],
                kx,
                (((1,), (1,)), ((), ())),
                preferred_element_type=F32,
            )
            w = jnp.exp2(score * (QK**-0.5 * math.log2(math.e)))
            if diagonal:
                pos = (at % rows) + lax.broadcasted_iota(jnp.int32, w.shape, 0)
                w = jnp.where(lax.broadcasted_iota(jnp.int32, w.shape, 1) <= pos, w, 0.0)
            pv = jnp.dot(w.astype(BF), vx, preferred_element_type=F32)
            if diagonal:
                acc[h, pl.ds(at, tall), :] = pv
            else:
                acc[h, pl.ds(at, tall), :] += pv
            return carry

        lax.fori_loop(lo * per_head, hi * per_head, step, 0, unroll=2)

    cuts = (0, heads // 2, heads)

    def attend_back(k, e):
        @pl.when(s >= k)
        def _():
            attend(s - k, False, cuts[e], cuts[e + 1])

    items = [(g, k) for g in range(ng) for k in range(1, n)]
    per = n - 1
    state = {"at": 0}

    def advance(g, part=1.0):
        to = min(len(items), g * per + math.ceil(part * per - 1e-6))
        for i in range(state["at"], to):
            stage1(*items[i])
            if i % per == AT and items[i][0] + LOOK < ng:
                own_send(items[i][0] + LOOK)
            if i >= LAG:
                stage2(*items[i - LAG])
            if i == len(items) - 1:
                for m in range(LAG):
                    stage2(*items[i - LAG + 1 + m])
        state["at"] = max(state["at"], to)

    def arrived(g):
        for k in range(1, n):
            stage3(g, k)

    for g in range(LOOK):
        own_send(g)
    for c in loads["tok"]:
        c.wait()

    gain = gain_r[...].reshape(1, width).astype(F32)

    def norm_step(i, carry):
        at = pl.ds(pl.multiple_of(i * 32, 32), 32)
        x = tok[at, :].astype(F32)
        r = lax.rsqrt(jnp.mean(x * x, axis=-1, keepdims=True) + EPS)
        normed[at, :] = (x * r * gain).astype(BF)
        return carry

    def norm_rows(lo, hi):
        lax.fori_loop(lo, hi, norm_step, 0)

    steps = rows // 32
    norm_rows(0, steps // 2)
    advance(0, 0.3)
    norm_rows(steps // 2, steps)
    advance(1, 0.6)
    arrived(0)

    lane = lax.broadcasted_iota(jnp.int32, (rows, LANES), 1)

    kv = jnp.dot(
        normed[...],
        gkv[...].reshape(width, 2 * LANES),
        preferred_element_type=F32,
    ).astype(BF)
    kbuf[s] = kv[:, :LANES]
    vbuf[s] = kv[:, LANES:]

    @pl.when(has_right)
    def _():
        for c in kvcopy(s):
            c.start()

    advance(3, 0.3)
    arrived(1)

    def q_step(h, carry):
        cols = pl.ds(pl.multiple_of(h * 2 * LANES, 2 * LANES), 2 * LANES)
        q = jnp.dot(normed[...], gq[:, :, cols].reshape(width, 2 * LANES), preferred_element_type=F32)
        for e in range(2):
            one = q[:, e * LANES : (e + 1) * LANES]
            q2[2 * h + e, :rows, :] = jnp.where(lane < QK, one, 0.0).astype(BF)
            q2[2 * h + e, rows:, :] = jnp.where(lane >= QK, one, 0.0).astype(BF)
        return carry

    lax.fori_loop(0, heads // 2, q_step, 0)

    def glu(i):
        cols = slice(i * WIDE, (i + 1) * WIDE)
        val = jnp.dot(normed[...], gb[i, :, :, :WIDE].reshape(width, WIDE), preferred_element_type=F32)
        gate = jnp.dot(normed[...], gb[i, :, :, WIDE:].reshape(width, WIDE), preferred_element_type=F32)
        g = (val * jax.nn.sigmoid(gate)).astype(BF)
        gated[:, cols] = g
        pad[RIM:, cols] = g.astype(F32)

    rim_copy = pltpu.make_async_remote_copy(
        gated.at[pl.ds(rows - RIM, RIM), :],
        rim,
        rims.at[0],
        rims.at[1],
        device_id=right,
        device_id_type=MESH,
    )

    taps = taps_r.shape[0]
    shift = RIM - (taps - 1)
    tile = min(128, rows)

    def conv_step(i, carry):
        cols = pl.ds(pl.multiple_of(i * LANES, LANES), LANES)
        for r in range(0, rows, tile):
            total = jnp.zeros((tile, LANES), F32)
            for j in range(taps):
                total = total + taps_r[j : j + 1, cols].astype(F32) * pad[
                    r + shift + j : r + shift + j + tile, cols
                ]
            conv[r : r + tile, cols] = total.astype(BF).astype(F32)
        return carry

    def convolve(i):
        lax.fori_loop(i * WIDE // LANES, (i + 1) * WIDE // LANES, conv_step, 0)

    def head_rows(i, carry):
        at = pl.multiple_of(i * tile, tile)
        ids = lax.broadcasted_iota(jnp.int32, (tile, LANES), 1)
        logs = jnp.zeros((tile, LANES), F32)
        for h in range(heads):
            a0 = acc[h, pl.ds(at, tile), :]
            a1 = acc[h, pl.ds(pl.multiple_of(rows + at, tile), tile), :]
            t0, t1 = a0[:, VDIM:], a1[:, VDIM:]
            diff = a0[:, :VDIM] / t0 - lam_r[h] * (a1[:, :VDIM] / t1)
            out = (
                diff
                * lax.rsqrt(jnp.mean(diff * diff, axis=-1, keepdims=True) + EPS)
                * hgain_r[...].astype(F32)
            )
            both[pl.ds(at, tile), h * VDIM : (h + 1) * VDIM] = out.astype(BF)
            logs = jnp.where(ids == 2 * h, jnp.log(t0), logs)
            logs = jnp.where(ids == 2 * h + 1, jnp.log(t1), logs)
        log_r[:, pl.ds(at, tile)] = logs.T[: 2 * heads, :]
        return carry

    def pcopy(i, o):
        return pltpu.make_async_remote_copy(
            part_out.at[i, o],
            part_in.at[i, o],
            ps.at[i, o],
            pr.at[i, o],
            device_id=mate,
            device_id_type=MESH,
        )

    mine = pl.ds(pl.multiple_of(t * half, half), half)
    other = pl.ds(pl.multiple_of((1 - t) * half, half), half)

    def out_block(i, o):
        part_out[i, o] = jnp.dot(both[other, :], gc[i, o], preferred_element_type=F32).astype(BF)
        pcopy(i, o).start()
        keep[i, o] = jnp.dot(both[mine, :], gc[i, o], preferred_element_type=F32)

    def finish(i):
        def go(o, carry):
            pcopy(i, o).wait_recv()
            pcopy(i, o).wait_send()
            mixed_r[:, pl.ds(pl.multiple_of((o * nc + i) * oc, oc), oc)] = (
                keep[i, o] + part_in[i, o].astype(F32)
            ).astype(BF)
            return carry

        lax.fori_loop(0, n, go, 0)

    attend(s, True, 0, heads)
    advance(4, 0.3)
    kv_take(1)
    attend_back(1, 0)
    attend_back(1, 1)
    advance(4, 0.6)
    arrived(2)
    glu(0)
    for i in range(1, nb):
        arrived(2 + i)
        glu(i)

    @pl.when(has_right)
    def _():
        rim_copy.start()

    if n > 2:
        kv_take(2)
        attend_back(2, 0)
        advance(4)
        attend_back(2, 1)
    advance(5, 0.3)
    for k in range(3, n):
        kv_take(k)

    @pl.when(has_left)
    def _():
        rim_copy.wait_recv()
        pad[:RIM, :] = rim[...].astype(F32)

    @pl.when(s == 0)
    def _():
        pad[:RIM, :] = jnp.zeros((RIM, chans), F32)

    for i in range(nb):
        convolve(i)
    cv = conv[...]
    sq_own[...] = jnp.broadcast_to(jnp.sum(cv * cv, axis=-1, keepdims=True), (rows, LANES))
    sq_copy = pltpu.make_async_remote_copy(
        sq_own, sq_in, sqs.at[0], sqs.at[1], device_id=mate, device_id_type=MESH
    )
    sq_copy.start()

    advance(5, 0.6)
    for k in range(3, n):
        attend_back(k, 0)
        attend_back(k, 1)
    advance(5)
    lax.fori_loop(0, rows // tile, head_rows, 0)
    sq_copy.wait()
    inv = lax.rsqrt((sq_own[:, :1] + sq_in[:, :1]) / conv_total + EPS)
    cgain = cgain_r[pl.ds(pl.multiple_of(t * chans, LANES), chans)].reshape(1, chans).astype(F32)
    both[:, att_rows:] = jax.nn.silu(conv[...] * inv * cgain).astype(BF)

    for i in range(nc):
        out_block(i, s)
    for i in range(nc - 1):
        for k in range(1, n):
            stage3(first_c + i, k)
            sides(k, lambda o, _: out_block(i, o))
    for i in range(nc - 1):
        finish(i)
    for k in range(1, n):
        stage3(ng - 1, k)
        sides(k, lambda o, _: out_block(nc - 1, o))
    finish(nc - 1)

    for g in range(ng):
        drain(g)

    @pl.when(has_right)
    def _():
        rim_copy.wait_send()
        for c in kvcopy(s):
            c.wait_send()

    for k in range(1, n):

        @pl.when((s >= k) & has_right)
        def _():
            for c in kvcopy(s - k):
                c.wait_send()


def body(n, conv_total, tokens, norm_gain, w_query, w_key, w_value, w_gv, w_gg, taps, cgain, hgain, lam, w_out):
    rows, width = tokens.shape
    heads = lam.shape[0]
    chans = w_gv.shape[1]
    qcols = w_query.shape[1]
    wrows = w_query.shape[0]
    ocols = w_out.shape[1]
    half = rows // 2
    nb = chans // WIDE
    nc = max(1, ocols // WIDE)
    oc = ocols // nc
    ng = 2 + nb + nc
    any_ = pl.BlockSpec(memory_space=pl.ANY)
    vm = pl.BlockSpec(memory_space=pltpu.VMEM)
    sm = pl.BlockSpec(memory_space=pltpu.SMEM)
    dma = pltpu.SemaphoreType.DMA
    v = pltpu.VMEM
    mixed, logs = pl.pallas_call(
        functools.partial(kernel, n, conv_total),
        out_shape=(
            jax.ShapeDtypeStruct((half, width), BF),
            jax.ShapeDtypeStruct((2 * heads, rows), F32),
        ),
        in_specs=[any_, vm, any_, any_, any_, any_, any_, vm, vm, vm, sm, any_],
        out_specs=(vm, vm),
        scratch_shapes=[
            v((rows, width), BF),
            v((rows, width), BF),
            v((n, wrows, 2 * LANES), BF),
            v((n, wrows, qcols), BF),
            v((nb, n, wrows, 2 * WIDE), BF),
            v((nc, n, heads * VDIM + chans, oc), BF),
            v((heads, 2 * rows, LANES), BF),
            v((n, rows, LANES), BF),
            v((n, rows, LANES), BF),
            v((heads, 2 * rows, 2 * VDIM), F32),
            v((rows, chans), BF),
            v((RIM, chans), BF),
            v((rows + RIM, chans), F32),
            v((rows, chans), F32),
            v((rows, LANES), F32),
            v((rows, LANES), F32),
            v((rows, heads * VDIM + chans), BF),
            v((nc, n, half, oc), BF),
            v((nc, n, half, oc), BF),
            v((nc, n, half, oc), F32),
            dma((4 + 2 * nb + 2 * nc,)),
            dma((ng, 2, n)),
            dma((ng, n)),
            dma((2, n)),
            dma((n,)),
            dma((ng, n)),
            dma((ng, n)),
            dma((ng, n)),
            dma((ng, n)),
            dma((ng, n)),
            dma((ng, n)),
            dma((ng, n)),
            dma((ng, n)),
            dma((2, n)),
            dma((2, n)),
            dma((2,)),
            dma((2,)),
            dma((nc, n)),
            dma((nc, n)),
        ],
        compiler_params=pltpu.CompilerParams(
            collective_id=0, has_side_effects=True, vmem_limit_bytes=60 * 1024 * 1024
        ),
    )(
        tokens,
        norm_gain,
        w_query,
        w_key,
        w_value,
        w_gv,
        w_gg,
        taps,
        cgain,
        hgain.reshape(1, -1),
        lam,
        w_out,
    )
    return mixed, logs.T


def solution(mesh):
    n = mesh.shape["sp"]

    def run(*args):
        return body(n, args[8].shape[0], *args)

    return jax.shard_map(
        run,
        mesh=mesh,
        in_specs=(
            P(("fs", "sp"), None),
            P(),
            P("sp", "tp"),
            P("sp", "tp"),
            P("sp", "tp"),
            P("sp", "tp"),
            P("sp", "tp"),
            P(None, "tp"),
            P(),
            P(),
            P("tp"),
            P(None, "sp"),
        ),
        out_specs=(P(("fs", "sp", "tp"), None), P(("fs", "sp"), "tp")),
        check_vma=False,
    )
```

```python
import functools
import math

import jax
import jax.numpy as jnp
from jax import lax
from jax.experimental import pallas as pl
from jax.experimental.pallas import tpu as pltpu
from jax.sharding import PartitionSpec as P

QK = 64
VDIM = 128
EPS = 1e-06
MESH = pl.DeviceIdType.MESH
BF = jnp.bfloat16
F32 = jnp.float32
LANES = 128
RIM = 32
LOOK = 2
LAG = 2
AT = 0
WIDE = 256


def kernel(
    n,
    conv_total,
    tok_h,
    gain_r,
    wq_h,
    wk_h,
    wv_h,
    wgv_h,
    wgg_h,
    taps_r,
    cgain_r,
    hgain_r,
    lam_r,
    wo_h,
    mixed_r,
    log_r,
    tok,
    normed,
    gkv,
    gq,
    gb,
    gc,
    q2,
    kbuf,
    vbuf,
    acc,
    gated,
    rim,
    pad,
    conv,
    sq_own,
    sq_in,
    both,
    part_out,
    part_in,
    keep,
    loc,
    zs,
    zr,
    zu,
    zv,
    xs,
    xr,
    ys,
    yr,
    hxs,
    hxr,
    hys,
    hyr,
    kvs,
    kvr,
    rims,
    sqs,
    ps,
    pr,
):
    s = lax.axis_index("sp")
    f = lax.axis_index("fs")
    t = lax.axis_index("tp")
    fx = f + 1 - 2 * (f % 2)
    fy = (f + 2) % 4
    left = {"sp": s - 1, "fs": f, "tp": t}
    right = {"sp": s + 1, "fs": f, "tp": t}
    xdev = {"sp": s, "fs": fx, "tp": t}
    ydev = {"sp": s, "fs": fy, "tp": t}
    mate = {"sp": s, "fs": f, "tp": 1 - t}
    rows, width = tok.shape
    heads = lam_r.shape[0]
    chans = gated.shape[1]
    qcols = wq_h.shape[1]
    half = rows // 2
    nb, nc, oc = gb.shape[0], gc.shape[0], gc.shape[3]
    groups = [(gkv, None), (gq, None)]
    groups += [(gb, i) for i in range(nb)] + [(gc, i) for i in range(nc)]
    first_c = 2 + nb
    ng = first_c + nc
    twice = ng - 1
    has_left = s > 0
    has_right = s < n - 1

    d_rows = wq_h.shape[0]
    att_rows = heads * VDIM
    loads = {}
    count = [0]

    def load(g, src, dst):
        c = pltpu.make_async_copy(src, dst, loc.at[count[0]])
        count[0] += 1
        loads.setdefault(g, []).append(c)
        c.start()

    load(0, wk_h, gkv.at[s, :, pl.ds(0, LANES)])
    load(0, wv_h, gkv.at[s, :, pl.ds(LANES, LANES)])
    load(1, wq_h, gq.at[s])
    load("tok", tok_h, tok)
    for i in range(nb):
        load(2 + i, wgv_h.at[:, pl.ds(i * WIDE, WIDE)], gb.at[i, s, :, pl.ds(0, WIDE)])
        load(2 + i, wgg_h.at[:, pl.ds(i * WIDE, WIDE)], gb.at[i, s, :, pl.ds(WIDE, WIDE)])
    for i in range(nc):
        cols = pl.ds(i * oc, oc)
        a_rows = pl.ds(pl.multiple_of(t * att_rows, att_rows), att_rows)
        c_rows = pl.ds(pl.multiple_of(2 * att_rows + t * chans, chans), chans)
        load(first_c + i, wo_h.at[a_rows, cols], gc.at[i, s, pl.ds(0, att_rows), :])
        load(first_c + i, wo_h.at[c_rows, cols], gc.at[i, s, pl.ds(att_rows, chans), :])

    bar = pltpu.get_barrier_semaphore()
    for dev in (xdev, ydev, mate):
        pl.semaphore_signal(bar, 1, device_id=dev, device_id_type=MESH)

    @pl.when(has_left)
    def _():
        pl.semaphore_signal(bar, 1, device_id=left, device_id_type=MESH)

    @pl.when(has_right)
    def _():
        pl.semaphore_signal(bar, 1, device_id=right, device_id_type=MESH)

    pl.semaphore_wait(bar, 3 + jnp.where(has_left, 1, 0) + jnp.where(has_right, 1, 0))

    def chunk(g, o, q, part=None):
        buf, i = groups[g]
        size = buf.shape[-2] // 4
        if part is not None:
            size = size // 2
            q = q * 2 + part
        at = pl.ds(pl.multiple_of(q * size, size), size)
        return buf.at[o, at, :] if i is None else buf.at[i, o, at, :]

    def zcopy(g, o, right_way):
        c = chunk(g, o, f)
        return pltpu.make_async_remote_copy(
            c,
            c,
            zs.at[g, 0 if right_way else 1, o],
            zr.at[g, o],
            device_id=right if right_way else left,
            device_id_type=MESH,
        )

    def xcopy(g, o, q):
        c = chunk(g, o, q)
        return pltpu.make_async_remote_copy(
            c, c, xs.at[g, o], xr.at[g, o], device_id=xdev, device_id_type=MESH
        )

    def ycopy(g, o, q):
        c = chunk(g, o, q)
        return pltpu.make_async_remote_copy(
            c, c, ys.at[g, o], yr.at[g, o], device_id=ydev, device_id_type=MESH
        )

    def hxcopy(g, o, q):
        c = chunk(g, o, q, 0)
        return pltpu.make_async_remote_copy(
            c, c, hxs.at[g, o], hxr.at[g, o], device_id=xdev, device_id_type=MESH
        )

    def hycopy(g, o, q):
        c = chunk(g, o, q, 1)
        return pltpu.make_async_remote_copy(
            c, c, hys.at[g, o], hyr.at[g, o], device_id=ydev, device_id_type=MESH
        )

    fd = 3 - f

    def ucopy(o, right_way):
        c = chunk(twice, o, fd)
        return pltpu.make_async_remote_copy(
            c,
            c,
            zu.at[0 if right_way else 1, o],
            zv.at[o],
            device_id=right if right_way else left,
            device_id_type=MESH,
        )

    def sides(k, fn):
        @pl.when(s >= k)
        def _():
            fn(s - k, True)

        @pl.when(s + k < n)
        def _():
            fn(s + k, False)

    def own_send(g):
        for c in loads[g]:
            c.wait()

        @pl.when(has_right)
        def _():
            zcopy(g, s, True).start()
            if g == twice:
                ucopy(s, True).start()

        @pl.when(has_left)
        def _():
            zcopy(g, s, False).start()
            if g == twice:
                ucopy(s, False).start()

    def stage1(g, k):
        def go(o, right_way):
            zcopy(g, o, right_way).wait_recv()
            xcopy(g, o, f).start()
            ycopy(g, o, f).start()

            @pl.when(has_right if right_way else has_left)
            def _():
                zcopy(g, o, right_way).start()

            if g == twice:
                ucopy(o, right_way).wait_recv()

                @pl.when(has_right if right_way else has_left)
                def _():
                    ucopy(o, right_way).start()

        sides(k, go)

    def stage2(g, k):
        if g == twice:
            return

        def go(o, right_way):
            xcopy(g, o, fx).wait_recv()
            hycopy(g, o, fx).start()
            ycopy(g, o, fy).wait_recv()
            hxcopy(g, o, fy).start()

        sides(k, go)

    def stage3(g, k):
        def go(o, right_way):
            if g == twice:
                xcopy(g, o, fx).wait_recv()
                ycopy(g, o, fy).wait_recv()
                return
            hxcopy(g, o, fd).wait_recv()
            hycopy(g, o, fd).wait_recv()

        sides(k, go)

    def drain(g):
        @pl.when(has_right)
        def _():
            zcopy(g, s, True).wait_send()
            if g == twice:
                ucopy(s, True).wait_send()

        @pl.when(has_left)
        def _():
            zcopy(g, s, False).wait_send()
            if g == twice:
                ucopy(s, False).wait_send()

        for k in range(1, n):

            def go(o, right_way):
                xcopy(g, o, f).wait_send()
                ycopy(g, o, f).wait_send()
                if g != twice:
                    hycopy(g, o, fx).wait_send()
                    hxcopy(g, o, fy).wait_send()

                @pl.when(has_right if right_way else has_left)
                def _():
                    zcopy(g, o, right_way).wait_send()
                    if g == twice:
                        ucopy(o, right_way).wait_send()

            sides(k, go)

    def kvcopy(o):
        return [
            pltpu.make_async_remote_copy(
                b.at[o], b.at[o], kvs.at[i, o], kvr.at[i, o], device_id=right, device_id_type=MESH
            )
            for i, b in enumerate((kbuf, vbuf))
        ]

    def kv_take(k):
        @pl.when(s >= k)
        def _():
            for c in kvcopy(s - k):
                c.wait_recv()

            @pl.when(has_right)
            def _():
                for c in kvcopy(s - k):
                    c.start()

    tall = min(256, rows)
    per_head = 2 * rows // tall

    def attend_self():
        for r in range(rows // tall):
            span = (r + 1) * tall
            vx = jnp.concatenate([vbuf[s, :span, :], jnp.ones((span, VDIM), BF)], axis=1)
            kx = kbuf[s, :span, :]

            def step(i, carry):
                h = i // 2
                at = pl.ds(pl.multiple_of((i % 2) * rows + r * tall, tall), tall)
                score = lax.dot_general(
                    q2[h, at, :],
                    kx,
                    (((1,), (1,)), ((), ())),
                    preferred_element_type=F32,
                )
                w = jnp.exp2(score * (QK**-0.5 * math.log2(math.e)))
                pos = r * tall + lax.broadcasted_iota(jnp.int32, w.shape, 0)
                w = jnp.where(lax.broadcasted_iota(jnp.int32, w.shape, 1) <= pos, w, 0.0)
                acc[h, at, :] = jnp.dot(w.astype(BF), vx, preferred_element_type=F32)
                return carry

            lax.fori_loop(0, 2 * heads, step, 0, unroll=2)

    def attend(o, diagonal, lo, hi):
        vx = jnp.concatenate([vbuf[o], jnp.ones((rows, VDIM), BF)], axis=1)
        kx = kbuf[o]

        def step(i, carry):
            h = i // per_head
            at = pl.multiple_of((i % per_head) * tall, tall)
            score = lax.dot_general(
                q2[h, pl.ds(at, tall), :],
                kx,
                (((1,), (1,)), ((), ())),
                preferred_element_type=F32,
            )
            w = jnp.exp2(score * (QK**-0.5 * math.log2(math.e)))
            if diagonal:
                pos = (at % rows) + lax.broadcasted_iota(jnp.int32, w.shape, 0)
                w = jnp.where(lax.broadcasted_iota(jnp.int32, w.shape, 1) <= pos, w, 0.0)
            pv = jnp.dot(w.astype(BF), vx, preferred_element_type=F32)
            if diagonal:
                acc[h, pl.ds(at, tall), :] = pv
            else:
                acc[h, pl.ds(at, tall), :] += pv
            return carry

        lax.fori_loop(lo * per_head, hi * per_head, step, 0, unroll=2)

    cuts = (0, heads // 2, heads)

    def attend_back(k, e):
        @pl.when(s >= k)
        def _():
            attend(s - k, False, cuts[e], cuts[e + 1])

    items = [(g, k) for g in range(ng) for k in range(1, n)]
    per = n - 1
    state = {"at": 0}

    def advance(g, part=1.0):
        to = min(len(items), g * per + math.ceil(part * per - 1e-6))
        for i in range(state["at"], to):
            stage1(*items[i])
            if i % per == AT and items[i][0] + LOOK < ng:
                own_send(items[i][0] + LOOK)
            if i >= LAG:
                stage2(*items[i - LAG])
            if i == len(items) - 1:
                for m in range(LAG):
                    stage2(*items[i - LAG + 1 + m])
        state["at"] = max(state["at"], to)

    def arrived(g):
        for k in range(1, n):
            stage3(g, k)

    for g in range(LOOK):
        own_send(g)
    for c in loads["tok"]:
        c.wait()

    gain = gain_r[...].reshape(1, width).astype(F32)

    def norm_step(i, carry):
        at = pl.ds(pl.multiple_of(i * 32, 32), 32)
        x = tok[at, :].astype(F32)
        r = lax.rsqrt(jnp.mean(x * x, axis=-1, keepdims=True) + EPS)
        normed[at, :] = (x * r * gain).astype(BF)
        return carry

    def norm_rows(lo, hi):
        lax.fori_loop(lo, hi, norm_step, 0)

    steps = rows // 32
    norm_rows(0, steps // 2)
    advance(0, 0.3)
    norm_rows(steps // 2, steps)
    advance(1, 0.6)
    arrived(0)

    lane = lax.broadcasted_iota(jnp.int32, (rows, LANES), 1)

    kv = jnp.dot(
        normed[...],
        gkv[...].reshape(width, 2 * LANES),
        preferred_element_type=F32,
    ).astype(BF)
    kbuf[s] = kv[:, :LANES]
    vbuf[s] = kv[:, LANES:]

    @pl.when(has_right)
    def _():
        for c in kvcopy(s):
            c.start()

    advance(3, 0.3)
    arrived(1)

    def q_step(h, carry):
        cols = pl.ds(pl.multiple_of(h * 2 * LANES, 2 * LANES), 2 * LANES)
        q = jnp.dot(normed[...], gq[:, :, cols].reshape(width, 2 * LANES), preferred_element_type=F32)
        for e in range(2):
            one = q[:, e * LANES : (e + 1) * LANES]
            q2[2 * h + e, :rows, :] = jnp.where(lane < QK, one, 0.0).astype(BF)
            q2[2 * h + e, rows:, :] = jnp.where(lane >= QK, one, 0.0).astype(BF)
        return carry

    lax.fori_loop(0, heads // 2, q_step, 0)

    def glu(i):
        cols = slice(i * WIDE, (i + 1) * WIDE)
        val = jnp.dot(normed[...], gb[i, :, :, :WIDE].reshape(width, WIDE), preferred_element_type=F32)
        gate = jnp.dot(normed[...], gb[i, :, :, WIDE:].reshape(width, WIDE), preferred_element_type=F32)
        g = (val * jax.nn.sigmoid(gate)).astype(BF)
        gated[:, cols] = g
        pad[RIM:, cols] = g.astype(F32)

    rim_copy = pltpu.make_async_remote_copy(
        gated.at[pl.ds(rows - RIM, RIM), :],
        rim,
        rims.at[0],
        rims.at[1],
        device_id=right,
        device_id_type=MESH,
    )

    taps = taps_r.shape[0]
    shift = RIM - (taps - 1)
    tile = min(128, rows)

    def conv_step(i, carry):
        cols = pl.ds(pl.multiple_of(i * LANES, LANES), LANES)
        for r in range(0, rows, tile):
            total = jnp.zeros((tile, LANES), F32)
            for j in range(taps):
                total = total + taps_r[j : j + 1, cols].astype(F32) * pad[
                    r + shift + j : r + shift + j + tile, cols
                ]
            conv[r : r + tile, cols] = total.astype(BF).astype(F32)
        return carry

    def convolve(i):
        lax.fori_loop(i * WIDE // LANES, (i + 1) * WIDE // LANES, conv_step, 0)

    def head_rows(i, carry):
        at = pl.multiple_of(i * tile, tile)
        ids = lax.broadcasted_iota(jnp.int32, (tile, LANES), 1)
        logs = jnp.zeros((tile, LANES), F32)
        for h in range(heads):
            a0 = acc[h, pl.ds(at, tile), :]
            a1 = acc[h, pl.ds(pl.multiple_of(rows + at, tile), tile), :]
            t0, t1 = a0[:, VDIM:], a1[:, VDIM:]
            diff = a0[:, :VDIM] / t0 - lam_r[h] * (a1[:, :VDIM] / t1)
            out = (
                diff
                * lax.rsqrt(jnp.mean(diff * diff, axis=-1, keepdims=True) + EPS)
                * hgain_r[...].astype(F32)
            )
            both[pl.ds(at, tile), h * VDIM : (h + 1) * VDIM] = out.astype(BF)
            logs = jnp.where(ids == 2 * h, jnp.log(t0), logs)
            logs = jnp.where(ids == 2 * h + 1, jnp.log(t1), logs)
        log_r[:, pl.ds(at, tile)] = logs.T[: 2 * heads, :]
        return carry

    def pcopy(i, o):
        return pltpu.make_async_remote_copy(
            part_out.at[i, o],
            part_in.at[i, o],
            ps.at[i, o],
            pr.at[i, o],
            device_id=mate,
            device_id_type=MESH,
        )

    mine = pl.ds(pl.multiple_of(t * half, half), half)
    other = pl.ds(pl.multiple_of((1 - t) * half, half), half)

    def out_block(i, o):
        part_out[i, o] = jnp.dot(both[other, :], gc[i, o], preferred_element_type=F32).astype(BF)
        pcopy(i, o).start()
        keep[i, o] = jnp.dot(both[mine, :], gc[i, o], preferred_element_type=F32)

    def finish(i):
        def go(o, carry):
            pcopy(i, o).wait_recv()
            pcopy(i, o).wait_send()
            mixed_r[:, pl.ds(pl.multiple_of((o * nc + i) * oc, oc), oc)] = (
                keep[i, o] + part_in[i, o].astype(F32)
            ).astype(BF)
            return carry

        lax.fori_loop(0, n, go, 0)

    attend_self()
    advance(4, 0.3)
    kv_take(1)
    attend_back(1, 0)
    attend_back(1, 1)
    advance(4, 0.6)
    arrived(2)
    glu(0)
    for i in range(1, nb):
        arrived(2 + i)
        glu(i)

    @pl.when(has_right)
    def _():
        rim_copy.start()

    if n > 2:
        kv_take(2)
        attend_back(2, 0)
        advance(4)
        attend_back(2, 1)
    advance(5, 0.3)
    for k in range(3, n):
        kv_take(k)

    @pl.when(has_left)
    def _():
        rim_copy.wait_recv()
        pad[:RIM, :] = rim[...].astype(F32)

    @pl.when(s == 0)
    def _():
        pad[:RIM, :] = jnp.zeros((RIM, chans), F32)

    for i in range(nb):
        convolve(i)
    cv = conv[...]
    sq_own[...] = jnp.broadcast_to(jnp.sum(cv * cv, axis=-1, keepdims=True), (rows, LANES))
    sq_copy = pltpu.make_async_remote_copy(
        sq_own, sq_in, sqs.at[0], sqs.at[1], device_id=mate, device_id_type=MESH
    )
    sq_copy.start()

    advance(5, 0.6)
    for k in range(3, n):
        attend_back(k, 0)
        attend_back(k, 1)
    advance(5)
    lax.fori_loop(0, rows // tile, head_rows, 0)
    sq_copy.wait()
    inv = lax.rsqrt((sq_own[:, :1] + sq_in[:, :1]) / conv_total + EPS)
    cgain = cgain_r[pl.ds(pl.multiple_of(t * chans, LANES), chans)].reshape(1, chans).astype(F32)
    both[:, att_rows:] = jax.nn.silu(conv[...] * inv * cgain).astype(BF)

    for i in range(nc):
        out_block(i, s)
    for i in range(nc - 1):
        for k in range(1, n):
            stage3(first_c + i, k)
            sides(k, lambda o, _: out_block(i, o))
    for i in range(nc - 1):
        finish(i)
    for k in range(1, n):
        stage3(ng - 1, k)
        sides(k, lambda o, _: out_block(nc - 1, o))
    finish(nc - 1)

    for g in range(ng):
        drain(g)

    @pl.when(has_right)
    def _():
        rim_copy.wait_send()
        for c in kvcopy(s):
            c.wait_send()

    for k in range(1, n):

        @pl.when((s >= k) & has_right)
        def _():
            for c in kvcopy(s - k):
                c.wait_send()


def body(n, conv_total, tokens, norm_gain, w_query, w_key, w_value, w_gv, w_gg, taps, cgain, hgain, lam, w_out):
    rows, width = tokens.shape
    heads = lam.shape[0]
    chans = w_gv.shape[1]
    qcols = w_query.shape[1]
    wrows = w_query.shape[0]
    ocols = w_out.shape[1]
    half = rows // 2
    nb = chans // WIDE
    nc = max(1, ocols // WIDE)
    oc = ocols // nc
    ng = 2 + nb + nc
    any_ = pl.BlockSpec(memory_space=pl.ANY)
    vm = pl.BlockSpec(memory_space=pltpu.VMEM)
    sm = pl.BlockSpec(memory_space=pltpu.SMEM)
    dma = pltpu.SemaphoreType.DMA
    v = pltpu.VMEM
    mixed, logs = pl.pallas_call(
        functools.partial(kernel, n, conv_total),
        out_shape=(
            jax.ShapeDtypeStruct((half, width), BF),
            jax.ShapeDtypeStruct((2 * heads, rows), F32),
        ),
        in_specs=[any_, vm, any_, any_, any_, any_, any_, vm, vm, vm, sm, any_],
        out_specs=(vm, vm),
        scratch_shapes=[
            v((rows, width), BF),
            v((rows, width), BF),
            v((n, wrows, 2 * LANES), BF),
            v((n, wrows, qcols), BF),
            v((nb, n, wrows, 2 * WIDE), BF),
            v((nc, n, heads * VDIM + chans, oc), BF),
            v((heads, 2 * rows, LANES), BF),
            v((n, rows, LANES), BF),
            v((n, rows, LANES), BF),
            v((heads, 2 * rows, 2 * VDIM), F32),
            v((rows, chans), BF),
            v((RIM, chans), BF),
            v((rows + RIM, chans), F32),
            v((rows, chans), F32),
            v((rows, LANES), F32),
            v((rows, LANES), F32),
            v((rows, heads * VDIM + chans), BF),
            v((nc, n, half, oc), BF),
            v((nc, n, half, oc), BF),
            v((nc, n, half, oc), F32),
            dma((4 + 2 * nb + 2 * nc,)),
            dma((ng, 2, n)),
            dma((ng, n)),
            dma((2, n)),
            dma((n,)),
            dma((ng, n)),
            dma((ng, n)),
            dma((ng, n)),
            dma((ng, n)),
            dma((ng, n)),
            dma((ng, n)),
            dma((ng, n)),
            dma((ng, n)),
            dma((2, n)),
            dma((2, n)),
            dma((2,)),
            dma((2,)),
            dma((nc, n)),
            dma((nc, n)),
        ],
        compiler_params=pltpu.CompilerParams(
            collective_id=0, has_side_effects=True, vmem_limit_bytes=60 * 1024 * 1024
        ),
    )(
        tokens,
        norm_gain,
        w_query,
        w_key,
        w_value,
        w_gv,
        w_gg,
        taps,
        cgain,
        hgain.reshape(1, -1),
        lam,
        w_out,
    )
    return mixed, logs.T


def solution(mesh):
    n = mesh.shape["sp"]

    def run(*args):
        return body(n, args[8].shape[0], *args)

    return jax.shard_map(
        run,
        mesh=mesh,
        in_specs=(
            P(("fs", "sp"), None),
            P(),
            P("sp", "tp"),
            P("sp", "tp"),
            P("sp", "tp"),
            P("sp", "tp"),
            P("sp", "tp"),
            P(None, "tp"),
            P(),
            P(),
            P("tp"),
            P(None, "sp"),
        ),
        out_specs=(P(("fs", "sp", "tp"), None), P(("fs", "sp"), "tp")),
        check_vma=False,
    )
```
